512 devices in a mesh: dp: 4 (over x), kv: 64 (over z, y), tp: 2 (over core).
Axes of the slice: x: 4, y: 8, z: 8, core: 2. Of those that a mesh axis runs over, the one named last changes fastest.
Arguments:
- tokens: bfloat16 [32, 1024], P('dp', 'kv'), may hold values from -6 to 6
- norm_gain: float32 [1024], P('kv'), may hold values from 0.1 to 1.9
- w_query: bfloat16 [1024, 4, 64], P('kv', 'tp'), may hold values from -0.1875 to 0.1875
- w_key: bfloat16 [1024, 4, 64], P('kv', 'tp'), may hold values from -0.1875 to 0.1875
- w_value: bfloat16 [1024, 4, 64], P('kv', 'tp'), may hold values from -0.1875 to 0.1875
- w_gate: bfloat16 [1024, 4, 64], P('kv', 'tp'), may hold values from -0.1875 to 0.1875
- w_forget: bfloat16 [1024, 4], P('kv', 'tp'), may hold values from -0.1875 to 0.1875
- w_out: bfloat16 [4, 64, 1024], P('tp', None, 'kv'), may hold values from -0.375 to 0.375
- cache_key: bfloat16 [32, 32768, 4, 64], P('dp', 'kv', 'tp'), may hold values from -6 to 6
- cache_value: bfloat16 [32, 32768, 4, 64], P('dp', 'kv', 'tp'), may hold values from -6 to 6
- cache_logf: float32 [32, 32768, 4], P('dp', 'kv', 'tp'), may hold values from -0.60003052 to 0, as said below
- lengths: int32 [32], P('dp'), may hold values from 31744 to 32767
Outputs:
- mixed: float32 [32, 1024], P('dp', 'kv')
- new_key: bfloat16 [32, 4, 64], P('dp', 'tp')
- new_value: float32 [32, 4, 64], P('dp', 'tp')
- new_logf: float32 [32, 4], P('dp', 'tp')
The draws below stay inside these ranges and needn't reach their ends.
Inputs may be any that keep to these rules, and one draw needn't show every extreme that they name: `lengths`: each sequence has between 31744 and 32767 cached tokens. `cache_logf`: log forget gates are at most 0; most are small (down to -1 / 32768, with a typical size that differs by head), and about six positions of each sequence and head hold drops of 0.2 to 0.6.
All inputs are finite; a program needn't handle non-finite values.
Results may differ from the reference program's by a relative error of at most 0.0095.
Values sent between devices are 32-bit elements.
A program may use at most 64 MiB of HBM per device.

```python
import math
import jax
import jax.numpy as jnp
from jax import lax

D = 1024
HEADS = 4
HEAD_DIM = 64
POS_DEV = 512
BATCH = 32
CTX = 32768


def draw_cache_logf(key, part):
    rate_key, spread_key, spike_key, height_key = jax.random.split(key, 4)
    head_rates = jnp.exp(jax.random.uniform(rate_key, (HEADS,), jnp.float32, math.log(0.05), math.log(0.5)))
    spread = jax.random.uniform(spread_key, (BATCH, CTX, HEADS), jnp.float32, 0.0, 2.0)
    spike_mask = jax.random.bernoulli(spike_key, 6.0 / CTX, (BATCH, CTX, HEADS))
    heights = jax.random.uniform(height_key, (BATCH, CTX, HEADS), jnp.float32, 0.2, 0.6)
    return -(spread * head_rates[None, None, :] / CTX) - jnp.where(spike_mask, heights, jnp.float32(0.0))


def place_ends(drawn, own_key, smallest, top_value):
    spot = [jax.random.randint(jax.random.fold_in(own_key, axis), (), 0, length) for axis, length in enumerate(drawn.shape)]
    main_axis = drawn.shape.index(max(drawn.shape))
    next_to = spot[:main_axis] + [(spot[main_axis] + 1) % drawn.shape[main_axis]] + spot[main_axis + 1:]
    return drawn.at[tuple(spot)].set(smallest).at[tuple(next_to)].set(top_value)


def shard_levels(rng, dims, cuts, least, top_value):
    level = 1.0
    for dim, shards_of in cuts:
        steps = jax.random.uniform(jax.random.fold_in(jax.random.fold_in(rng, 6), dim), (shards_of,), jnp.float32, least / len(cuts), top_value / len(cuts))
        level = level * jnp.repeat(jnp.exp(steps), dims[dim] // shards_of).reshape((-1,) + (1,) * (len(dims) - 1 - dim))
    return level


def noise(rng, shape, deviation, limit, cuts=(), kind=jnp.bfloat16):
    factor_of = shard_levels(rng, shape, cuts, -0.22, 0.18) if cuts else 1.0
    drawn = jax.random.normal(rng, shape, jnp.float32) * deviation * factor_of
    return jnp.minimum(jnp.maximum(drawn, -limit), limit).astype(kind)


def setup_inputs(seed: int = 0) -> dict:
    arg_keys = jax.random.split(jax.random.key(seed), 13)
    tokens = noise(arg_keys[0], (BATCH, D), 1.0, 6.0, ((0, 4), (1, 64)))
    norm_gain = jnp.clip(1.0 + 0.18 * jax.random.normal(arg_keys[1], (D,), jnp.float32), 0.1, 1.9)
    w_query = noise(arg_keys[2], (D, HEADS, HEAD_DIM), D ** -0.5, 0.1875, ((0, 64), (1, 2)))
    w_key = noise(arg_keys[3], (D, HEADS, HEAD_DIM), D ** -0.5, 0.1875, ((0, 64), (1, 2)))
    w_value = noise(arg_keys[4], (D, HEADS, HEAD_DIM), D ** -0.5, 0.1875, ((0, 64), (1, 2)))
    w_gate = noise(arg_keys[5], (D, HEADS, HEAD_DIM), D ** -0.5, 0.1875, ((0, 64), (1, 2)))
    w_forget = noise(arg_keys[6], (D, HEADS), D ** -0.5, 0.1875, ((0, 64), (1, 2)))
    w_out = noise(arg_keys[7], (HEADS, HEAD_DIM, D), (HEADS * HEAD_DIM) ** -0.5, 0.375, ((0, 2), (2, 64)))
    cache_key = noise(arg_keys[8], (BATCH, CTX, HEADS, HEAD_DIM), 1.0, 6.0, ((0, 4), (1, 64), (2, 2)))
    cache_value = noise(arg_keys[9], (BATCH, CTX, HEADS, HEAD_DIM), 1.0, 6.0, ((0, 4), (1, 64), (2, 2)))
    cache_logf = draw_cache_logf(jax.random.fold_in(arg_keys[12], 71), 0)
    lengths = place_ends(jax.random.randint(arg_keys[11], (BATCH,), CTX - 2 * POS_DEV, CTX), jax.random.fold_in(arg_keys[11], 1), CTX - 2 * POS_DEV, CTX - 1).astype(jnp.int32)
    return dict(tokens=tokens, norm_gain=norm_gain, w_query=w_query, w_key=w_key, w_value=w_value, w_gate=w_gate, w_forget=w_forget, w_out=w_out, cache_key=cache_key, cache_value=cache_value, cache_logf=cache_logf, lengths=lengths)


eps = 1e-06
very_low = -1e+30

def head_norm(values):
    return values * lax.rsqrt(lax.optimization_barrier(jnp.mean(values * values, axis=-1, keepdims=True)) + eps)

def one_sequence(packed):
    query_vec, key_new, value_new, logf_new, keys_all, values_all, logf_all, length = packed
    positions = jnp.arange(keys_all.shape[0], dtype=jnp.int32)
    in_range = positions < length
    masked_logf = jnp.where(in_range[:, None], logf_all, jnp.float32(0.0))
    running = jnp.cumsum(masked_logf, axis=0)
    later_sum = running[-1][None, :] - running
    forget_bias = logf_new[None, :] + later_sum
    wide_query = query_vec.astype(jnp.float32)
    scores = jnp.einsum('he,she->hs', wide_query, keys_all.astype(jnp.float32)) * HEAD_DIM ** (-0.5) + forget_bias.T
    score_new = lax.optimization_barrier(jnp.sum(wide_query * key_new.astype(jnp.float32), axis=-1)) * HEAD_DIM ** (-0.5)
    peak = jnp.maximum(lax.optimization_barrier(jnp.max(jnp.where(in_range[None, :], scores, very_low), axis=-1)), score_new)
    weights = jnp.where(in_range[None, :], jnp.exp(scores - peak[:, None]), jnp.float32(0.0))
    weight_new = jnp.exp(score_new - peak)
    denominator = lax.optimization_barrier(jnp.sum(weights, axis=-1)) + weight_new
    weighted = jnp.einsum('hs,she->he', weights.astype(jnp.bfloat16).astype(jnp.float32), values_all.astype(jnp.float32))
    weighted = weighted + weight_new[:, None] * value_new
    return weighted / denominator[:, None]

def reference(tokens, norm_gain, w_query, w_key, w_value, w_gate, w_forget, w_out, cache_key, cache_value, cache_logf, lengths):
    wide_tokens = tokens.astype(jnp.float32)
    inv_root = lax.rsqrt(lax.optimization_barrier(jnp.mean(wide_tokens * wide_tokens, axis=-1, keepdims=True)) + eps)
    normed = (wide_tokens * inv_root * norm_gain).astype(jnp.bfloat16)
    wide_normed = normed.astype(jnp.float32)

    def project(weight):
        return jnp.einsum('bd,dhe->bhe', wide_normed, weight.astype(jnp.float32))
    query_vec = head_norm(project(w_query)).astype(jnp.bfloat16)
    key_new = head_norm(project(w_key)).astype(jnp.bfloat16)
    value_new = project(w_value)
    gate_silu = jax.nn.silu(project(w_gate))
    logf_new = jax.nn.log_sigmoid(jnp.dot(normed, w_forget, preferred_element_type=jnp.float32))
    attended = lax.map(one_sequence, (query_vec, key_new, value_new, logf_new, cache_key, cache_value, cache_logf, lengths))
    gated = (head_norm(attended) * gate_silu).astype(jnp.bfloat16)
    mixed = jnp.einsum('bhe,hed->bd', gated.astype(jnp.float32), w_out.astype(jnp.float32))
    return (mixed, key_new, value_new, logf_new)
```

```python
import jax
import jax.numpy as jnp
from jax import lax
from jax.experimental import pallas as pl
from jax.experimental.pallas import tpu as pltpu
from jax.sharding import Mesh
from jax.sharding import PartitionSpec as P

D = 1024
HD = 64
N = 8
KV = ("kv_0", "kv_1")
EPS = 1e-6
MESH = pl.DeviceIdType.MESH
FAR_FIRST = (4, 3, 5, 2, 6, 1, 7)
HI = lax.Precision.HIGHEST


def iota(shape, axis):
    return lax.broadcasted_iota(jnp.int32, shape, axis)


def lane_sum(x):
    return jnp.sum(x, axis=1, keepdims=True)


def to_row(cols):
    sub, lane = iota((8, 128), 0), iota((8, 128), 1)
    tile = jnp.zeros((8, 128), jnp.float32)
    for c, col in enumerate(cols):
        tile = jnp.where(lane == 8 * c + sub, col, tile)
    return jnp.sum(tile, axis=0, keepdims=True)


def from_row(row, c):
    sub, lane = iota((8, 128), 0), iota((8, 128), 1)
    return lane_sum(jnp.where(lane == 8 * c + sub, row, 0.0))


def by_head(first, second):
    return jnp.where(iota((8, 128), 1) < HD, first, second)


def head_mean(x):
    left = lane_sum(jnp.where(iota((8, 128), 1) < HD, x, 0.0))
    right = lane_sum(jnp.where(iota((8, 128), 1) < HD, 0.0, x))
    return by_head(left, right) * (1.0 / HD)


def kernel(
    tok_h, gain_h, wq_h, wk_h, wv_h, wg_h, wf_h, wo_h, key_h, val_h, logf_h, len_h,
    mixed_o, nkey_o, nval_o, nlogf_o,
    tok, gain, wq, wk, wv, wg, wf, wo, key, val, logf, lens, small_sem, logf_sem, key_sem, val_sem,
    crit, rs_src, rs, ar, ag, tpb, bias_s, side, send_sem, recv_sem,
):
    z, y, t = lax.axis_index("kv_0"), lax.axis_index("kv_1"), lax.axis_index("tp")
    barrier = pltpu.get_barrier_semaphore()
    for d in FAR_FIRST:
        pl.semaphore_signal(barrier, 1, device_id={"kv_1": lax.rem(y + d, N)}, device_id_type=MESH)
        pl.semaphore_signal(barrier, 1, device_id={"kv_0": lax.rem(z + d, N)}, device_id_type=MESH)
    pl.semaphore_signal(barrier, 1, device_id={"tp": 1 - t}, device_id_type=MESH)

    smalls = [
        pltpu.make_async_copy(a, b, small_sem.at[i])
        for i, (a, b) in enumerate(
            [(tok_h, tok), (gain_h, gain), (wq_h, wq), (wk_h, wk), (wv_h, wv), (wg_h, wg), (wf_h, wf),
             (len_h, lens), (wo_h, wo)]
        )
    ]
    for copy in smalls:
        copy.start()
    logf_copy = pltpu.make_async_copy(logf_h, logf, logf_sem)
    logf_copy.start()
    key_copies = [
        pltpu.make_async_copy(key_h.at[pl.ds(i * 256, 256)], key.at[pl.ds(i * 256, 256)], key_sem.at[i])
        for i in range(4)
    ]
    val_copies = [
        pltpu.make_async_copy(val_h.at[pl.ds(i * 256, 256)], val.at[pl.ds(i * 256, 256)], val_sem.at[i])
        for i in range(4)
    ]
    for copy in key_copies + val_copies:
        copy.start()

    def exchange(stage, buf, src, axis, me):
        for d in FAR_FIRST:
            pltpu.make_async_remote_copy(
                src, buf.at[me], send_sem.at[stage], recv_sem.at[stage],
                device_id={axis: lax.rem(me + d, N)}, device_id_type=MESH,
            ).start()

    def arrived(stage, buf):
        seven = buf.at[pl.ds(0, N - 1)]
        pltpu.make_async_copy(seven, seven, recv_sem.at[stage]).wait()

    def sent(stage, buf):
        seven = buf.at[pl.ds(0, N - 1)]
        pltpu.make_async_copy(seven, seven, send_sem.at[stage]).wait()

    for copy in smalls:
        copy.wait()
    wide = tok[...].astype(jnp.float32)
    squares = lane_sum(wide * wide)
    scaled = wide * gain[...]
    narrow = scaled.astype(jnp.bfloat16)

    def project(w):
        w32 = w[...].astype(jnp.float32)
        halves = [
            jnp.dot(narrow, w32[:, h, :].astype(jnp.bfloat16), preferred_element_type=jnp.float32)
            for h in range(2)
        ]
        return jnp.concatenate(halves, axis=1)

    wf32 = wf[...].astype(jnp.float32)
    narrow32 = narrow.astype(jnp.float32)
    forget = [lane_sum(narrow32 * wf32[h : h + 1, :]) for h in range(2)]

    sub8, lane8 = iota((8, 8), 0), iota((8, 8), 1)
    len_col = lane_sum(jnp.where(sub8 == lane8, lens[...].astype(jnp.float32), 0.0))
    len_col = jnp.concatenate([len_col, len_col], axis=0)
    first = (z * N + y) * 512
    position = (iota((16, 512), 1) + first).astype(jnp.float32)
    valid = position < len_col
    logf_copy.wait()
    gates = jnp.concatenate([logf[:, 0, :], logf[:, 1, :]], axis=0)
    gates = jnp.where(valid, gates, 0.0)
    blocks = jnp.concatenate([gates[:, 128 * j : 128 * (j + 1)] for j in range(4)], axis=0)
    row_i, col_i = iota((128, 256), 0), iota((128, 256), 1)
    after = jnp.where((col_i >= 128) | (row_i > col_i), 1.0, 0.0).astype(jnp.float32)
    sums = jnp.dot(blocks, after, preferred_element_type=jnp.float32, precision=HI)
    later = jnp.zeros((16, 128), jnp.float32)
    for j in (3, 2, 1, 0):
        bias_s[:, 128 * j : 128 * (j + 1)] = sums[16 * j : 16 * (j + 1), :128] + later
        later = later + sums[16 * j : 16 * (j + 1), 128:]

    crit[0, y, 0:8, :] = project(wq)
    crit[0, y, 8:9, :] = to_row([squares, forget[0], forget[1], later[:8], later[8:]])
    pieces = [project(wk), project(wv), project(wg)]
    for j in range(N):
        for i, piece in enumerate(pieces):
            rs_src[j, :, 128 * i : 128 * (i + 1)] = piece[j : j + 1, :]

    pl.semaphore_wait(barrier, 15)
    exchange(0, crit.at[0], crit.at[0, y], "kv_1", y)
    for d in FAR_FIRST:
        other = lax.rem(y + d, N)
        pltpu.make_async_remote_copy(
            rs_src.at[other], rs.at[y], send_sem.at[4], recv_sem.at[4],
            device_id={"kv_1": other}, device_id_type=MESH,
        ).start()
    rs[y] = rs_src[y]

    def total(stage):
        acc = crit[stage, 0]
        for j in range(1, N):
            acc = acc + crit[stage, j]
        return acc

    def later_rows(stage, me):
        acc = jnp.zeros((1, 128), jnp.float32)
        for j in range(1, N):
            acc = acc + jnp.where(j > me, crit[stage, j, 8:9, :], 0.0)
        return acc

    arrived(0, crit.at[0])
    crit[1, z] = total(0)
    exchange(1, crit.at[1], crit.at[1, z], "kv_0", z)

    arrived(4, rs)
    row = rs[0]
    for j in range(1, N):
        row = row + rs[j]
    ar[z] = row
    exchange(5, ar, ar.at[z], "kv_0", z)

    later_y = later_rows(0, y)
    for copy in key_copies:
        copy.wait()

    arrived(1, crit.at[1])
    summed = total(1)
    info = summed[8:9, :]
    q_sum = summed[0:8, :]
    mean_square = from_row(info, 0) * (1.0 / D)
    inv_square = 1.0 / (mean_square + EPS)
    inv_root = lax.rsqrt(mean_square + EPS)
    q_mean = head_mean(q_sum * q_sum)
    query = q_sum * (inv_root * lax.rsqrt(q_mean * inv_square + EPS))
    query = query.astype(jnp.bfloat16)
    side[0] = query.astype(jnp.float32)
    new_logf = []
    for h in range(2):
        logit = from_row(info, 1 + h) * inv_root
        new_logf.append(jnp.minimum(logit, 0.0) - jnp.log1p(jnp.exp(-jnp.abs(logit))))
    later_all = later_y + later_rows(1, z)
    extra = jnp.concatenate([from_row(later_all, 3) + new_logf[0], from_row(later_all, 4) + new_logf[1]], axis=0)

    q32 = side[0]
    double = jnp.concatenate([q32, q32], axis=0)
    row16, lane16 = iota((16, 128), 0), iota((16, 128), 1)
    own_head = (row16 // 8) == (lane16 // HD)
    lhs = jnp.concatenate(
        [jnp.where(own_head & (row16 % 8 == b), double, 0.0).astype(jnp.bfloat16) for b in range(8)], axis=1
    )
    scores = jnp.dot(lhs, key[...], preferred_element_type=jnp.float32) * (HD ** -0.5)
    weights = jnp.where(valid, jnp.exp(scores + (bias_s[...] + extra)), 0.0)
    den = lane_sum(weights)
    for copy in val_copies:
        copy.wait()
    wide_out = lax.dot_general(
        weights.astype(jnp.bfloat16), val[...], (((1,), (1,)), ((), ())), preferred_element_type=jnp.float32
    )
    acc = jnp.zeros((16, 128), jnp.float32)
    for b in range(8):
        acc = jnp.where(own_head & (row16 % 8 == b), wide_out[:, 128 * b : 128 * (b + 1)], acc)
    crit[2, y, 0:8, :] = acc[:8] + acc[8:]
    crit[2, y, 8:9, :] = to_row([den[:8], den[8:]])
    exchange(2, crit.at[2], crit.at[2, y], "kv_1", y)

    arrived(5, ar)
    row = ar[0]
    for j in range(1, N):
        row = row + ar[j]
    ag[y] = row
    exchange(6, ag, ag.at[y], "kv_1", y)

    arrived(2, crit.at[2])
    crit[3, z] = total(2)
    exchange(3, crit.at[3], crit.at[3, z], "kv_0", z)

    arrived(6, ag)
    everything = jnp.concatenate([ag[j] for j in range(N)], axis=0)
    k_sum = everything[:, 0:128]
    value_new = everything[:, 128:256] * inv_root
    gate = everything[:, 256:384] * inv_root
    k_mean = head_mean(k_sum * k_sum)
    key_new = (k_sum * (inv_root * lax.rsqrt(k_mean * inv_square + EPS))).astype(jnp.bfloat16)
    key_new32 = key_new.astype(jnp.float32)
    silu = gate * jax.nn.sigmoid(gate)
    score_new = head_mean(side[0] * key_new32) * (HD ** 0.5)
    weight_new = jnp.exp(score_new)
    nkey_o[...] = key_new32
    nval_o[...] = value_new
    nlogf_o[...] = by_head(new_logf[0], new_logf[1])

    arrived(3, crit.at[3])
    summed = total(3)
    info = summed[8:9, :]
    denominator = by_head(from_row(info, 0), from_row(info, 1)) + weight_new
    attended = (summed[0:8, :] + weight_new * value_new) / denominator
    gated = attended * lax.rsqrt(head_mean(attended * attended) + EPS) * silu
    gated = gated.astype(jnp.bfloat16)
    mine = lax.dot_general(
        gated[:, :HD], wo[0], (((1,), (1,)), ((), ())), preferred_element_type=jnp.float32
    ) + lax.dot_general(
        gated[:, HD:], wo[1], (((1,), (1,)), ((), ())), preferred_element_type=jnp.float32
    )
    tpb[t] = mine
    last = pltpu.make_async_remote_copy(
        tpb.at[t], tpb.at[t], send_sem.at[7], recv_sem.at[7], device_id={"tp": 1 - t}, device_id_type=MESH
    )
    last.start()
    for stage in range(4):
        sent(stage, crit.at[stage])
    sent(4, rs)
    sent(5, ar)
    sent(6, ag)
    last.wait()
    mixed_o[...] = tpb[0] + tpb[1]


def on_device(tokens, norm_gain, w_query, w_key, w_value, w_gate, w_forget, w_out, cache_key, cache_value, cache_logf, lengths):
    span = cache_key.shape[1]
    keys = jnp.transpose(cache_key, (0, 2, 3, 1)).reshape(8 * 2 * HD, span)
    values = jnp.transpose(cache_value, (0, 2, 3, 1)).reshape(8 * 2 * HD, span)
    logf = jnp.transpose(cache_logf, (0, 2, 1))
    args = (
        tokens, norm_gain.reshape(1, -1), w_query, w_key, w_value, w_gate, w_forget.T,
        jnp.transpose(w_out, (0, 2, 1)), keys, values, logf, lengths.reshape(1, -1),
    )
    f32 = jnp.float32
    tile = jax.ShapeDtypeStruct((8, 128), f32)
    scratch = [pltpu.VMEM(a.shape, a.dtype) for a in args] + [
        pltpu.SemaphoreType.DMA((9,)),
        pltpu.SemaphoreType.DMA(()),
        pltpu.SemaphoreType.DMA((4,)),
        pltpu.SemaphoreType.DMA((4,)),
        pltpu.VMEM((4, N, 9, 128), f32),
        pltpu.VMEM((N, 1, 384), f32),
        pltpu.VMEM((N, 1, 384), f32),
        pltpu.VMEM((N, 1, 384), f32),
        pltpu.VMEM((N, 1, 384), f32),
        pltpu.VMEM((2, 8, 16), f32),
        pltpu.VMEM((16, 512), f32),
        pltpu.VMEM((1, 8, 128), f32),
        pltpu.SemaphoreType.DMA((8,)),
        pltpu.SemaphoreType.DMA((8,)),
    ]
    mixed, nkey, nval, nlogf = pl.pallas_call(
        kernel,
        out_shape=(jax.ShapeDtypeStruct((8, 16), f32), tile, tile, tile),
        in_specs=[pl.BlockSpec(memory_space=pltpu.HBM)] * 12,
        out_specs=tuple(pl.BlockSpec(memory_space=pltpu.VMEM) for _ in range(4)),
        scratch_shapes=scratch,
        compiler_params=pltpu.CompilerParams(collective_id=0, has_side_effects=True),
        name="decode_step",
    )(*args)
    key_new = nkey.reshape(8, 2, HD).astype(jnp.bfloat16)
    value_new = nval.reshape(8, 2, HD)
    return mixed, key_new, value_new, nlogf.reshape(8, 2, HD)[:, :, 0]


def solution(mesh):
    finer = Mesh(
        mesh.devices.reshape(mesh.shape["dp"], N, N, mesh.shape["tp"]), ("dp", "kv_0", "kv_1", "tp")
    )
    return jax.shard_map(
        on_device,
        mesh=finer,
        in_specs=(
            P("dp", KV), P(KV), P(KV, "tp", None), P(KV, "tp", None), P(KV, "tp", None), P(KV, "tp", None),
            P(KV, "tp"), P("tp", None, KV), P("dp", KV, "tp", None), P("dp", KV, "tp", None),
            P("dp", KV, "tp"), P("dp"),
        ),
        out_specs=(P("dp", KV), P("dp", "tp", None), P("dp", "tp", None), P("dp", "tp")),
        check_vma=False,
    )
```

```python
import jax
import jax.numpy as jnp
from jax import lax
from jax.experimental import pallas as pl
from jax.experimental.pallas import tpu as pltpu
from jax.sharding import Mesh
from jax.sharding import PartitionSpec as P

D = 1024
HD = 64
N = 8
KV = ("kv_0", "kv_1")
EPS = 1e-6
MESH = pl.DeviceIdType.MESH
FAR_FIRST = (4, 3, 5, 2, 6, 1, 7)
HI = lax.Precision.HIGHEST


def iota(shape, axis):
    return lax.broadcasted_iota(jnp.int32, shape, axis)


def lane_sum(x):
    return jnp.sum(x, axis=1, keepdims=True)


def to_row(cols):
    sub, lane = iota((8, 128), 0), iota((8, 128), 1)
    tile = jnp.zeros((8, 128), jnp.float32)
    for c, col in enumerate(cols):
        tile = jnp.where(lane == 8 * c + sub, col, tile)
    return jnp.sum(tile, axis=0, keepdims=True)


def from_row(row, c):
    sub, lane = iota((8, 128), 0), iota((8, 128), 1)
    return lane_sum(jnp.where(lane == 8 * c + sub, row, 0.0))


def by_head(first, second):
    return jnp.where(iota((8, 128), 1) < HD, first, second)


def head_mean(x):
    left = lane_sum(jnp.where(iota((8, 128), 1) < HD, x, 0.0))
    right = lane_sum(jnp.where(iota((8, 128), 1) < HD, 0.0, x))
    return by_head(left, right) * (1.0 / HD)


def kernel(
    tok_h, gain_h, wq_h, wk_h, wv_h, wg_h, wf_h, wo_h, key_h, val_h, logf_h, len_h,
    mixed_o, nkey_o, nval_o, nlogf_o,
    tok, gain, wq, wk, wv, wg, wf, wo, key, val, logf, lens, small_sem, key_sem, val_sem,
    crit, rs_src, rs, ar, ag, tpb, bias_s, side, send_sem, recv_sem,
):
    z, y, t = lax.axis_index("kv_0"), lax.axis_index("kv_1"), lax.axis_index("tp")
    smalls = [
        pltpu.make_async_copy(a, b, small_sem.at[i])
        for i, (a, b) in enumerate(
            [(tok_h, tok), (gain_h, gain), (wq_h, wq), (wf_h, wf), (wk_h, wk), (wv_h, wv), (wg_h, wg),
             (len_h, lens), (logf_h, logf), (wo_h, wo)]
        )
    ]
    for copy in smalls[:4]:
        copy.start()
    barrier = pltpu.get_barrier_semaphore()
    for d in FAR_FIRST:
        pl.semaphore_signal(barrier, 1, device_id={"kv_1": (y + d) & 7}, device_id_type=MESH)
        pl.semaphore_signal(barrier, 1, device_id={"kv_0": (z + d) & 7}, device_id_type=MESH)
    pl.semaphore_signal(barrier, 1, device_id={"tp": 1 - t}, device_id_type=MESH)
    for copy in smalls[4:]:
        copy.start()
    key_copies = [
        pltpu.make_async_copy(key_h.at[pl.ds(i * 256, 256)], key.at[pl.ds(i * 256, 256)], key_sem.at[i])
        for i in range(4)
    ]
    val_copies = [
        pltpu.make_async_copy(val_h.at[pl.ds(i * 256, 256)], val.at[pl.ds(i * 256, 256)], val_sem.at[i])
        for i in range(4)
    ]
    for copy in key_copies + val_copies:
        copy.start()

    def exchange(stage, buf, src, axis, me):
        for d in FAR_FIRST:
            pltpu.make_async_remote_copy(
                src, buf.at[me], send_sem.at[stage], recv_sem.at[stage],
                device_id={axis: (me + d) & 7}, device_id_type=MESH,
            ).start()

    def arrived(stage, buf):
        seven = buf.at[pl.ds(0, N - 1)]
        pltpu.make_async_copy(seven, seven, recv_sem.at[stage]).wait()

    def sent(stage, buf):
        seven = buf.at[pl.ds(0, N - 1)]
        pltpu.make_async_copy(seven, seven, send_sem.at[stage]).wait()

    for copy in smalls[:4]:
        copy.wait()
    wide = tok[...].astype(jnp.float32)
    squares = lane_sum(wide * wide)
    scaled = wide * gain[...]
    narrow = scaled.astype(jnp.bfloat16)

    def project(w):
        w32 = w[...].astype(jnp.float32)
        halves = [
            jnp.dot(narrow, w32[:, h, :].astype(jnp.bfloat16), preferred_element_type=jnp.float32)
            for h in range(2)
        ]
        return jnp.concatenate(halves, axis=1)

    wf32 = wf[...].astype(jnp.float32)
    narrow32 = narrow.astype(jnp.float32)
    forget = [lane_sum(narrow32 * wf32[h : h + 1, :]) for h in range(2)]
    crit[0, y, 0:8, :] = project(wq)
    crit[0, y, 8:9, :] = to_row([squares, forget[0], forget[1]])
    pl.semaphore_wait(barrier, 15)
    exchange(0, crit.at[0], crit.at[0, y], "kv_1", y)

    for copy in smalls[4:]:
        copy.wait()
    sub8, lane8 = iota((8, 8), 0), iota((8, 8), 1)
    len_col = lane_sum(jnp.where(sub8 == lane8, lens[...].astype(jnp.float32), 0.0))
    len_col = jnp.concatenate([len_col, len_col], axis=0)
    first = (z * N + y) * 512
    position = (iota((16, 512), 1) + first).astype(jnp.float32)
    valid = position < len_col
    gates = jnp.concatenate([logf[:, 0, :], logf[:, 1, :]], axis=0)
    gates = jnp.where(valid, gates, 0.0)
    blocks = jnp.concatenate([gates[:, 128 * j : 128 * (j + 1)] for j in range(4)], axis=0)
    row_i, col_i = iota((128, 256), 0), iota((128, 256), 1)
    after = jnp.where((col_i >= 128) | (row_i > col_i), 1.0, 0.0).astype(jnp.float32)
    sums = jnp.dot(blocks, after, preferred_element_type=jnp.float32, precision=HI)
    later = jnp.zeros((16, 128), jnp.float32)
    for j in (3, 2, 1, 0):
        bias_s[:, 128 * j : 128 * (j + 1)] = sums[16 * j : 16 * (j + 1), :128] + later
        later = later + sums[16 * j : 16 * (j + 1), 128:]
    pieces = [project(wk), project(wv), project(wg)]
    shard_row = to_row([later[:8], later[8:]])
    for j in range(N):
        for i, piece in enumerate(pieces):
            rs_src[j, :, 128 * i : 128 * (i + 1)] = piece[j : j + 1, :]
        rs_src[j, :, 384:512] = shard_row
    for d in FAR_FIRST:
        other = (y + d) & 7
        pltpu.make_async_remote_copy(
            rs_src.at[other], rs.at[y], send_sem.at[4], recv_sem.at[4],
            device_id={"kv_1": other}, device_id_type=MESH,
        ).start()
    rs[y] = rs_src[y]

    def total(stage):
        acc = crit[stage, 0]
        for j in range(1, N):
            acc = acc + crit[stage, j]
        return acc

    def later_rows(buf, me):
        acc = jnp.zeros((1, 128), jnp.float32)
        for j in range(1, N):
            acc = acc + jnp.where(j > me, buf[j, :, 384:512], 0.0)
        return acc

    arrived(0, crit.at[0])
    crit[1, z] = total(0)
    exchange(1, crit.at[1], crit.at[1, z], "kv_0", z)

    arrived(4, rs)
    row = rs[0]
    for j in range(1, N):
        row = row + rs[j]
    ar[z] = row
    exchange(5, ar, ar.at[z], "kv_0", z)

    later_y = later_rows(rs, y)
    for copy in key_copies:
        copy.wait()

    arrived(1, crit.at[1])
    summed = total(1)
    info = summed[8:9, :]
    q_sum = summed[0:8, :]
    mean_square = from_row(info, 0) * (1.0 / D)
    inv_square = 1.0 / (mean_square + EPS)
    inv_root = lax.rsqrt(mean_square + EPS)
    q_mean = head_mean(q_sum * q_sum)
    query = q_sum * (inv_root * lax.rsqrt(q_mean * inv_square + EPS))
    query = query.astype(jnp.bfloat16)
    side[0] = query.astype(jnp.float32)
    new_logf = []
    for h in range(2):
        logit = from_row(info, 1 + h) * inv_root
        new_logf.append(jnp.minimum(logit, 0.0) - jnp.log1p(jnp.exp(-jnp.abs(logit))))

    q32 = side[0]
    double = jnp.concatenate([q32, q32], axis=0)
    row16, lane16 = iota((16, 128), 0), iota((16, 128), 1)
    own_head = (row16 // 8) == (lane16 // HD)
    lhs = jnp.concatenate(
        [jnp.where(own_head & (row16 % 8 == b), double, 0.0).astype(jnp.bfloat16) for b in range(8)], axis=1
    )
    scores = jnp.dot(lhs, key[...], preferred_element_type=jnp.float32) * (HD ** -0.5)
    weights = jnp.where(valid, jnp.exp(scores + bias_s[...]), 0.0)
    den = lane_sum(weights)
    for copy in val_copies:
        copy.wait()
    wide_out = lax.dot_general(
        weights.astype(jnp.bfloat16), val[...], (((1,), (1,)), ((), ())), preferred_element_type=jnp.float32
    )
    acc = jnp.zeros((16, 128), jnp.float32)
    for b in range(8):
        acc = jnp.where(own_head & (row16 % 8 == b), wide_out[:, 128 * b : 128 * (b + 1)], acc)
    arrived(5, ar)
    later_all = later_y + later_rows(ar, z)
    decay = [jnp.exp(from_row(later_all, h) + new_logf[h]) for h in range(2)]
    crit[2, y, 0:8, :] = (acc[:8] + acc[8:]) * by_head(decay[0], decay[1])
    crit[2, y, 8:9, :] = to_row([den[:8] * decay[0], den[8:] * decay[1]])
    exchange(2, crit.at[2], crit.at[2, y], "kv_1", y)

    row = ar[0]
    for j in range(1, N):
        row = row + ar[j]
    ag[y] = row
    exchange(6, ag, ag.at[y], "kv_1", y)

    arrived(2, crit.at[2])
    crit[3, z] = total(2)
    exchange(3, crit.at[3], crit.at[3, z], "kv_0", z)

    arrived(6, ag)
    everything = jnp.concatenate([ag[j] for j in range(N)], axis=0)
    k_sum = everything[:, 0:128]
    value_new = everything[:, 128:256] * inv_root
    gate = everything[:, 256:384] * inv_root
    k_mean = head_mean(k_sum * k_sum)
    key_new = (k_sum * (inv_root * lax.rsqrt(k_mean * inv_square + EPS))).astype(jnp.bfloat16)
    key_new32 = key_new.astype(jnp.float32)
    silu = gate * jax.nn.sigmoid(gate)
    score_new = head_mean(side[0] * key_new32) * (HD ** 0.5)
    weight_new = jnp.exp(score_new)
    for h in range(2):
        nval_o[:, h, :] = value_new[:, HD * h : HD * (h + 1)]
        nlogf_o[h : h + 1, :] = to_row([new_logf[h]])[:, :8]
    nkey_o[...] = jnp.stack([key_new32[:, :HD], key_new32[:, HD:]], axis=1).astype(jnp.bfloat16)

    arrived(3, crit.at[3])
    summed = total(3)
    info = summed[8:9, :]
    denominator = by_head(from_row(info, 0), from_row(info, 1)) + weight_new
    attended = (summed[0:8, :] + weight_new * value_new) / denominator
    gated = attended * lax.rsqrt(head_mean(attended * attended) + EPS) * silu
    gated = gated.astype(jnp.bfloat16)
    mine = lax.dot_general(
        gated[:, :HD], wo[0], (((1,), (1,)), ((), ())), preferred_element_type=jnp.float32
    ) + lax.dot_general(
        gated[:, HD:], wo[1], (((1,), (1,)), ((), ())), preferred_element_type=jnp.float32
    )
    tpb[t] = mine
    last = pltpu.make_async_remote_copy(
        tpb.at[t], tpb.at[t], send_sem.at[7], recv_sem.at[7], device_id={"tp": 1 - t}, device_id_type=MESH
    )
    last.start()
    for stage in range(4):
        sent(stage, crit.at[stage])
    sent(4, rs)
    sent(5, ar)
    sent(6, ag)
    last.wait()
    mixed_o[...] = tpb[0] + tpb[1]


def write_out(a, b, c, d, a_h, b_h, c_h, d_h, sem):
    copies = [
        pltpu.make_async_copy(src, dst, sem.at[i])
        for i, (src, dst) in enumerate([(a, a_h), (b, b_h), (c, c_h), (d, d_h)])
    ]
    for copy in copies:
        copy.start()
    for copy in copies:
        copy.wait()


def on_device(tokens, norm_gain, w_query, w_key, w_value, w_gate, w_forget, w_out, cache_key, cache_value, cache_logf, lengths):
    span = cache_key.shape[1]
    keys = jnp.transpose(cache_key, (0, 2, 3, 1)).reshape(8 * 2 * HD, span)
    values = jnp.transpose(cache_value, (0, 2, 3, 1)).reshape(8 * 2 * HD, span)
    logf = jnp.transpose(cache_logf, (0, 2, 1))
    args = (
        tokens, norm_gain.reshape(1, -1), w_query, w_key, w_value, w_gate, w_forget.T,
        jnp.transpose(w_out, (0, 2, 1)), keys, values, logf, lengths.reshape(1, -1),
    )
    f32 = jnp.float32
    tile = jax.ShapeDtypeStruct((8, 128), f32)
    scratch = [pltpu.VMEM(a.shape, a.dtype) for a in args] + [
        pltpu.SemaphoreType.DMA((10,)),
        pltpu.SemaphoreType.DMA((4,)),
        pltpu.SemaphoreType.DMA((4,)),
        pltpu.VMEM((4, N, 9, 128), f32),
        pltpu.VMEM((N, 1, 512), f32),
        pltpu.VMEM((N, 1, 512), f32),
        pltpu.VMEM((N, 1, 512), f32),
        pltpu.VMEM((N, 1, 512), f32),
        pltpu.VMEM((2, 8, 16), f32),
        pltpu.VMEM((16, 512), f32),
        pltpu.VMEM((1, 8, 128), f32),
        pltpu.SemaphoreType.DMA((8,)),
        pltpu.SemaphoreType.DMA((8,)),
    ]
    shapes = [((8, 16), f32), ((8, 2, HD), jnp.bfloat16), ((8, 2, HD), f32), ((2, 8), f32)]
    results = pl.pallas_call(
        kernel,
        out_shape=tuple(pltpu.VMEM(*a) for a in shapes),
        in_specs=[pl.BlockSpec(memory_space=pltpu.HBM)] * 12,
        out_specs=tuple(pl.BlockSpec(memory_space=pltpu.VMEM) for _ in shapes),
        scratch_shapes=scratch,
        compiler_params=pltpu.CompilerParams(collective_id=0, has_side_effects=True),
        name="decode_step",
    )(*args)
    mixed, key_new, value_new, logf_new = pl.pallas_call(
        write_out,
        out_shape=tuple(jax.ShapeDtypeStruct(*a) for a in shapes),
        in_specs=[pl.BlockSpec(memory_space=pltpu.VMEM)] * 4,
        out_specs=tuple(pl.BlockSpec(memory_space=pltpu.HBM) for _ in shapes),
        scratch_shapes=[pltpu.SemaphoreType.DMA((4,))],
        name="write_out",
    )(*(pltpu.with_memory_space_constraint(r, pltpu.VMEM) for r in results))
    return mixed, key_new, value_new, logf_new.T


def solution(mesh):
    finer = Mesh(
        mesh.devices.reshape(mesh.shape["dp"], N, N, mesh.shape["tp"]), ("dp", "kv_0", "kv_1", "tp")
    )
    return jax.shard_map(
        on_device,
        mesh=finer,
        in_specs=(
            P("dp", KV), P(KV), P(KV, "tp", None), P(KV, "tp", None), P(KV, "tp", None), P(KV, "tp", None),
            P(KV, "tp"), P("tp", None, KV), P("dp", KV, "tp", None), P("dp", KV, "tp", None),
            P("dp", KV, "tp"), P("dp"),
        ),
        out_specs=(P("dp", KV), P("dp", "tp", None), P("dp", "tp", None), P("dp", "tp")),
        check_vma=False,
    )
```
